32 devices in a mesh: ep: 8 (over z, x), tp: 4 (over y, core).
Axes of the slice: x: 2, y: 2, z: 4, core: 2. Of those that a mesh axis runs over, the one named last changes fastest.
Arguments:
- mixer_input: bfloat16 [2048, 2048], P('ep'), may hold values from -6 to 6
- mixer_gain: float32 [2048], replicated, may hold values from 0.1 to 8
- query_one: bfloat16 [2048, 512], P(None, 'tp'), may hold values from -0.1875 to 0.1875
- query_two: bfloat16 [2048, 512], P(None, 'tp'), may hold values from -0.1875 to 0.1875
- key_one: bfloat16 [2048, 256], P(None, 'tp'), may hold values from -0.1875 to 0.1875
- key_two: bfloat16 [2048, 256], P(None, 'tp'), may hold values from -0.1875 to 0.1875
- value_weight: bfloat16 [2048, 512], P(None, 'tp'), may hold values from -0.125 to 0.125
- lambdas: float32 [8], P('tp'), may hold values from 0.3 to 0.8
- head_gain: float32 [128], replicated, may hold values from 0.1 to 1.9
- output_weight: bfloat16 [1024, 2048], P('tp'), may hold values from -0.1875 to 0.1875
- expert_input: bfloat16 [4096, 2048], P(('ep', 'tp')), may hold values from -6 to 6
- expert_gain: float32 [2048], replicated, may hold values from 0.1 to 1.9
- routes: int32 [4096, 2], P(('ep', 'tp')), may hold values from 0 to 7, all different within a row; in each aligned block of 128 rows (0 to 127, 128 to 255, ...) at most 40 rows name the same one
- route_weight: float32 [4096, 2], P(('ep', 'tp')), may hold values from 0.2 to 1
- expert_gate: bfloat16 [8, 2048, 1024], P('ep', None, 'tp'), may hold values from -0.125 to 0.125
- expert_up: bfloat16 [8, 2048, 1024], P('ep', None, 'tp'), may hold values from -0.125 to 0.125
- expert_down: bfloat16 [8, 1024, 2048], P('ep', 'tp'), may hold values from -0.1875 to 0.1875
- shared_gate: bfloat16 [2048, 512], P(None, 'tp'), may hold values from -0.125 to 0.125
- shared_up: bfloat16 [2048, 512], P(None, 'tp'), may hold values from -0.125 to 0.125
- shared_down: bfloat16 [512, 2048], P('tp'), may hold values from -0.25 to 0.25
Outputs:
- mixer_output: bfloat16 [2048, 2048], P(('ep', 'tp'))
- expert_output: bfloat16 [4096, 2048], P(('ep', 'tp'))
The draws below stay inside these ranges and needn't reach their ends.
Inputs may be any that keep to these rules, and one draw needn't show every extreme that they name: `routes`: each row names 2 different experts; in the rows of one device no expert is named by more than 40 rows, and some device names some expert exactly 40 times.
All inputs are finite; a program needn't handle non-finite values.
Results may differ from the reference program's by a relative error of at most 0.014.
The reference program's roundings to bfloat16 on the way count: a program that leaves them out, or rounds other values in their place, can miss the bound.
Values may be sent and summed in bfloat16 or wider, within the bound.
A program may use at most 128 MiB of HBM per device.

```python
import math
import jax
import jax.numpy as jnp
import numpy as np
from jax import lax

D = 2048
HEADS = 8
KV_HEADS = 4
HEAD = 64
VDIM = 128
EFF = 1024
SFF = 512
TOP = 2
EXPERTS = 8
ROWS = 128
CAP = 40
SEQ_LEN = 2048
TOKENS = 4096
N_EP = 8
N_TP = 4


def draw_mixer_gain(key, part):
    return jnp.clip(1.0 + 0.18 * jax.random.normal(key, (D,), jnp.float32), 0.1, 1.9)


def shard_levels(stream_key, shape, cuts, least, largest):
    def one(position, blocks):
        draws = jax.random.uniform(jax.random.fold_in(jax.random.fold_in(stream_key, 6), position), (blocks,), jnp.float32, least / len(cuts), largest / len(cuts))
        return jnp.repeat(jnp.exp(draws), shape[position] // blocks).reshape((-1,) + (1,) * (len(shape) - position - 1))

    level = one(*cuts[0])
    for cut in cuts[1:]:
        level = level * one(*cut)
    return level


def deal_out(own_key, own, number, rows, number_of, top, most, slope):
    sequence = jax.random.permutation(own_key, number_of)
    crowded, common = shares(number_of, rows * top, most, slope, True), shares(number_of, rows * top, most, slope, False)
    places = jnp.arange(number_of)

    def named(tallies, offset_by):
        used = int((tallies > 0).sum())
        fixed = max(1, used // 4)
        moved = fixed + (places - fixed + offset_by * (used - fixed)) % max(1, number_of - fixed)
        return jnp.zeros((number_of,), jnp.int32).at[sequence[jnp.where(places < fixed, places, moved)]].set(jnp.asarray(tallies, jnp.int32))

    tallies = jnp.where(number % 4 == 0, named(crowded, number // 4), named(common, number - number // 4 - 1))
    mixed = jax.random.permutation(jax.random.fold_in(own, 3), number_of)
    giver, sink = mixed[0:number_of // 2 * 2:2], mixed[1:number_of // 2 * 2:2]
    slack = jnp.minimum(tallies[giver] - 1, most - tallies[sink]) // 2
    slack = jnp.where((giver == sequence[0]) | (sink == sequence[0]) | (tallies[sink] == 0), 0, jnp.maximum(slack, 0))
    moved = jax.random.randint(jax.random.fold_in(own, 4), (number_of // 2,), 0, 1 << 20) % (slack + 1)
    tallies = tallies.at[giver].add(-moved).at[sink].add(moved)
    items = jnp.searchsorted(jnp.cumsum(tallies), jnp.arange(rows * top), side="right").astype(jnp.int32)
    listing = items.reshape(top, rows).T
    listing = listing[jax.random.permutation(jax.random.fold_in(own, 1), rows)]
    offset_by = jax.random.randint(jax.random.fold_in(own, 2), (rows, 1), 0, top)
    return jnp.take_along_axis(listing, (jnp.arange(top)[None, :] + offset_by) % top, axis=1)


def shares(count, total, reach, slope, full):
    loads = [(1 << 20) // math.isqrt(standing ** slope) + 1 for standing in range(1, count + 1)]
    largest = reach if full else min(reach, max(-(-total // count), total * loads[0] // sum(loads)))
    least = 1 if total - largest >= count - 1 else 0
    given, surplus = [largest] + [least] * (count - 1), total - largest - least * (count - 1)
    while surplus > 0:
        free = [i for i in range(1, count) if given[i] < largest] or [i for i in range(1, count) if given[i] < reach]
        whole, budget = sum([loads[i] for i in free]), surplus
        for i in free:
            extra = min(reach - given[i], max(1, budget * loads[i] // whole), surplus)
            given[i] = given[i] + extra
            surplus = surplus - extra
    return np.array(given)


def centred(rng, dims, width, most, shards=(), kind=jnp.bfloat16):
    drawn = width * jax.random.normal(rng, dims, jnp.float32)
    if shards:
        drawn = drawn * shard_levels(rng, dims, shards, -0.22, 0.18)
    return jnp.clip(drawn, -most, most).astype(kind)


def setup_inputs(seed: int = 0) -> dict:
    arg_keys = jax.random.split(jax.random.key(seed), 21)
    mixer_input = centred(arg_keys[0], (SEQ_LEN, D), 1.0, 6.0, ((0, 8),))
    mixer_gain = draw_mixer_gain(jax.random.fold_in(arg_keys[20], 71), 0)
    query_one = centred(arg_keys[2], (D, HEADS * HEAD), (D // 2) ** -0.5, 0.1875, ((1, 4),))
    query_two = centred(arg_keys[3], (D, HEADS * HEAD), (D // 2) ** -0.5, 0.1875, ((1, 4),))
    key_one = centred(arg_keys[4], (D, KV_HEADS * HEAD), (D // 2) ** -0.5, 0.1875, ((1, 4),))
    key_two = centred(arg_keys[5], (D, KV_HEADS * HEAD), (D // 2) ** -0.5, 0.1875, ((1, 4),))
    value_weight = centred(arg_keys[6], (D, KV_HEADS * VDIM), D ** -0.5, 0.125, ((1, 4),))
    lambdas = jnp.clip(0.3 + 0.5 * jax.random.uniform(arg_keys[7], (HEADS,), jnp.float32) ** shard_levels(arg_keys[7], (HEADS,), ((0, 4),), -0.2, 0.2), 0.3, 0.8)
    head_gain = jnp.clip(1.0 + 0.18 * jax.random.normal(arg_keys[8], (VDIM,), jnp.float32), 0.1, 1.9)
    output_weight = centred(arg_keys[9], (HEADS * VDIM, D), (HEADS * VDIM) ** -0.5, 0.1875, ((0, 4),))
    expert_input = centred(arg_keys[10], (TOKENS, D), 1.0, 6.0, ((0, 32),))
    expert_gain = jnp.clip(1.0 + 0.18 * jax.random.normal(arg_keys[11], (D,), jnp.float32), 0.1, 1.9)
    routes_keys = jax.random.split(jax.random.fold_in(arg_keys[12], 1), TOKENS // ROWS)
    routes_turns = jax.random.permutation(jax.random.fold_in(arg_keys[12], 3), TOKENS // ROWS)
    routes = jax.vmap(lambda own, number: deal_out(jax.random.fold_in(arg_keys[12], 2), own, number, ROWS, EXPERTS, TOP, CAP, 2))(routes_keys, routes_turns).reshape((TOKENS, TOP))
    route_weight = jnp.clip(jnp.exp(math.log(1.0) - 1.609438 * jax.random.uniform(arg_keys[13], (TOKENS, TOP), jnp.float32) ** shard_levels(arg_keys[13], (TOKENS, TOP), ((0, 32),), -0.2, 0.2)), 0.2, 1.0)
    expert_gate = centred(arg_keys[14], (EXPERTS, D, EFF), D ** -0.5, 0.125, ((0, 8), (2, 4)))
    expert_up = centred(arg_keys[15], (EXPERTS, D, EFF), D ** -0.5, 0.125, ((0, 8), (2, 4)))
    expert_down = centred(arg_keys[16], (EXPERTS, EFF, D), EFF ** -0.5, 0.1875, ((0, 8), (1, 4)))
    shared_gate = centred(arg_keys[17], (D, SFF), D ** -0.5, 0.125, ((1, 4),))
    shared_up = centred(arg_keys[18], (D, SFF), D ** -0.5, 0.125, ((1, 4),))
    shared_down = centred(arg_keys[19], (SFF, D), SFF ** -0.5, 0.25, ((0, 4),))
    return dict(mixer_input=mixer_input, mixer_gain=mixer_gain, query_one=query_one, query_two=query_two, key_one=key_one, key_two=key_two, value_weight=value_weight, lambdas=lambdas, head_gain=head_gain, output_weight=output_weight, expert_input=expert_input, expert_gain=expert_gain, routes=routes, route_weight=route_weight, expert_gate=expert_gate, expert_up=expert_up, expert_down=expert_down, shared_gate=shared_gate, shared_up=shared_up, shared_down=shared_down)


EPS = 1e-06
NEG = -1e+30

def normalize(activations, scaling):
    values = activations.astype(jnp.float32)
    factor = lax.rsqrt(lax.optimization_barrier(jnp.mean(values * values, axis=-1, keepdims=True)) + EPS)
    return (values * factor * scaling).astype(jnp.bfloat16)

def swiglu(inputs, gate_weight, up_weight):
    gated = jnp.dot(inputs, gate_weight, preferred_element_type=jnp.float32)
    lifted = jnp.dot(inputs, up_weight, preferred_element_type=jnp.float32)
    return (jax.nn.silu(gated) * lifted).astype(jnp.bfloat16)

def quarter_sum(hidden, down_weight):
    group_width = hidden.shape[1] // N_TP
    running_sum = jnp.zeros((hidden.shape[0], down_weight.shape[1]), jnp.float32)
    for group_index in range(N_TP):
        partial_product = jnp.dot(hidden[:, group_index * group_width:(group_index + 1) * group_width], down_weight[group_index * group_width:(group_index + 1) * group_width], preferred_element_type=jnp.float32)
        rounded = lax.optimization_barrier(partial_product.astype(jnp.bfloat16))
        running_sum = running_sum + rounded.astype(jnp.float32)
    return running_sum

def attention(mixer_input, mixer_gain, query_one, query_two, key_one, key_two, value_weight, lambdas, head_gain, output_weight):
    normed = normalize(mixer_input, mixer_gain)
    tokens = normed.shape[0]
    group_size = HEADS // KV_HEADS

    def project(weight):
        return jnp.dot(normed, weight, preferred_element_type=jnp.float32).astype(jnp.bfloat16)
    query_first = project(query_one).reshape(tokens, KV_HEADS, group_size, HEAD)
    query_second = project(query_two).reshape(tokens, KV_HEADS, group_size, HEAD)
    key_first = project(key_one).reshape(tokens, KV_HEADS, HEAD).astype(jnp.float32)
    key_second = project(key_two).reshape(tokens, KV_HEADS, HEAD).astype(jnp.float32)
    value_rows = project(value_weight).reshape(tokens, KV_HEADS, VDIM).astype(jnp.float32)
    lambda_grid = lambdas.reshape(KV_HEADS, group_size)[:, :, None, None]
    key_pos = jnp.arange(tokens, dtype=jnp.int32)
    span_rows = min(128, tokens)

    def single_map(queries, key_rows, visible):
        scores = jnp.einsum('qkgd,jkd->kgqj', queries.astype(jnp.float32), key_rows) * HEAD ** (-0.5)
        scores = jnp.where(visible, scores, NEG)
        highest = lax.optimization_barrier(jnp.max(scores, axis=-1, keepdims=True))
        weights = jnp.where(visible, jnp.exp(scores - highest), 0.0)
        totals = lax.optimization_barrier(jnp.sum(weights, axis=-1))
        rounded = lax.optimization_barrier(weights.astype(jnp.bfloat16)).astype(jnp.float32)
        mixed = jnp.einsum('kgqj,jkd->kgqd', rounded, value_rows)
        return mixed / totals[..., None]

    def query_block(block_index):
        offset = (block_index * span_rows).astype(jnp.int32)
        query_pos = offset + jnp.arange(span_rows, dtype=jnp.int32)
        visible = key_pos[None, :] <= query_pos[:, None]
        first_part = single_map(lax.dynamic_slice_in_dim(query_first, offset, span_rows, 0), key_first, visible)
        second_part = single_map(lax.dynamic_slice_in_dim(query_second, offset, span_rows, 0), key_second, visible)
        combined = first_part - lambda_grid * second_part
        factor = lax.rsqrt(lax.optimization_barrier(jnp.mean(combined * combined, axis=-1, keepdims=True)) + EPS)
        normed_heads = (combined * factor * head_gain).astype(jnp.bfloat16)
        return normed_heads.transpose(2, 0, 1, 3).reshape(span_rows, HEADS * VDIM)
    head_rows = lax.map(query_block, jnp.arange(tokens // span_rows, dtype=jnp.int32))
    head_rows = head_rows.reshape(tokens, HEADS * VDIM)
    return quarter_sum(head_rows, output_weight).astype(jnp.bfloat16)

def experts_part(expert_input, expert_gain, routes, route_weight, expert_gate, expert_up, expert_down, shared_gate, shared_up, shared_down):
    normed = normalize(expert_input, expert_gain)
    tokens = normed.shape[0]
    shared_result = quarter_sum(swiglu(normed, shared_gate, shared_up), shared_down)
    flat_routes = routes.reshape(-1).astype(jnp.int32)
    copies = flat_routes.shape[0]
    onehot = (flat_routes[:, None] == jnp.arange(EXPERTS, dtype=jnp.int32)[None, :]).astype(jnp.int32)
    slot_place = lax.optimization_barrier(jnp.sum((jnp.cumsum(onehot, axis=0) - onehot) * onehot, axis=1)).astype(jnp.int32)
    owners = (jnp.arange(copies, dtype=jnp.int32) // TOP).astype(jnp.int32)
    table = jnp.zeros((EXPERTS, N_EP * N_TP * CAP), jnp.int32).at[flat_routes, slot_place].set(owners)

    def one_expert(expert_index):
        chosen = normed[table[expert_index]]
        hidden = swiglu(chosen, expert_gate[expert_index], expert_up[expert_index])
        return quarter_sum(hidden, expert_down[expert_index]).astype(jnp.bfloat16)
    results = lax.map(one_expert, jnp.arange(EXPERTS, dtype=jnp.int32))
    picked = results[flat_routes, slot_place].astype(jnp.float32).reshape(tokens, TOP, -1)
    routed = lax.optimization_barrier(jnp.sum(picked * route_weight[:, :, None], axis=1))
    return (routed + shared_result).astype(jnp.bfloat16)

def reference(mixer_input, mixer_gain, query_one, query_two, key_one, key_two, value_weight, lambdas, head_gain, output_weight, expert_input, expert_gain, routes, route_weight, expert_gate, expert_up, expert_down, shared_gate, shared_up, shared_down):
    mixer_output = attention(mixer_input, mixer_gain, query_one, query_two, key_one, key_two, value_weight, lambdas, head_gain, output_weight)
    expert_output = experts_part(expert_input, expert_gain, routes, route_weight, expert_gate, expert_up, expert_down, shared_gate, shared_up, shared_down)
    return (mixer_output, expert_output)
```

```python
import functools
import math

import jax
import jax.numpy as jnp
from jax import lax
from jax.experimental import pallas as pl
from jax.experimental.pallas import tpu as pltpu
from jax.sharding import PartitionSpec as P

HEAD = 64


EPS = 1e-06
NEG = -1e30
GROUPS = 4


def normalize(activations, scaling):
    values = activations.astype(jnp.float32)
    factor = lax.rsqrt(jnp.mean(values * values, axis=-1, keepdims=True) + EPS)
    return (values * factor * scaling).astype(jnp.bfloat16)


def attention_kernel(
    shape, rank_ref, lambdas_ref, queries_ref, keys_ref, gain_ref, out_ref, maxima, totals, weighted
):
    rows, chunk, local_kv, group, value_dim = shape
    rank = rank_ref[0]
    maxima[...] = jnp.full(maxima.shape, NEG, jnp.float32)
    totals[...] = jnp.zeros(totals.shape, jnp.float32)
    weighted[...] = jnp.zeros(weighted.shape, jnp.float32)
    heads = local_kv * group
    key_cols = local_kv * HEAD
    chunks = rows // chunk
    scale = HEAD**-0.5 * math.log2(math.e)

    def block(index, masked):
        start = pl.multiple_of(index * rows, rows)
        for kv in range(local_kv):
            value_start = 2 * key_cols + kv * value_dim
            for part in range(chunks):
                span = (part + 1) * chunk if masked else rows
                values = keys_ref[pl.ds(start, span), value_start : value_start + value_dim]
                for which in range(2):
                    first = which * key_cols + kv * HEAD
                    keys = keys_ref[pl.ds(start, span), first : first + HEAD]
                    for g in range(group):
                        head = kv * group + g
                        col = (which * heads + head) * HEAD
                        queries = queries_ref[part * chunk : (part + 1) * chunk, col : col + HEAD]
                        scores = lax.dot_general(
                            queries,
                            keys,
                            (((1,), (1,)), ((), ())),
                            preferred_element_type=jnp.float32,
                        )
                        if masked:
                            row = part * chunk + lax.broadcasted_iota(jnp.int32, scores.shape, 0)
                            col_pos = lax.broadcasted_iota(jnp.int32, scores.shape, 1)
                            scores = jnp.where(col_pos <= row, scores, NEG)
                        slot = (which * heads + head) * chunks + part
                        earlier = maxima[slot]
                        latest = jnp.maximum(earlier, jnp.max(scores, axis=1, keepdims=True))
                        shrink = jnp.exp2((earlier - latest) * scale)
                        weights = jnp.exp2((scores - latest[:, :1]) * scale)
                        totals[slot] = totals[slot] * shrink + jnp.sum(
                            weights, axis=1, keepdims=True
                        )
                        weighted[slot] = weighted[slot] * shrink[:, :1] + jnp.dot(
                            weights.astype(jnp.bfloat16),
                            values,
                            preferred_element_type=jnp.float32,
                        )
                        maxima[slot] = latest

    def earlier_block(index, carry):
        block(index, False)
        return carry

    lax.fori_loop(0, rank, earlier_block, 0)
    block(rank, True)
    for head in range(heads):
        for part in range(chunks):
            one = head * chunks + part
            two = (heads + head) * chunks + part
            combined = (
                weighted[one] / totals[one][:, :1]
                - lambdas_ref[head] * (weighted[two] / totals[two][:, :1])
            )
            factor = lax.rsqrt(jnp.mean(combined * combined, axis=1, keepdims=True) + EPS)
            out_ref[
                part * chunk : (part + 1) * chunk, head * value_dim : (head + 1) * value_dim
            ] = (combined * factor * gain_ref[...]).astype(jnp.bfloat16)


def attention(queries, keys, rank, lambdas, head_gain, local_kv, group):
    rows = queries.shape[0]
    value_dim = head_gain.shape[0]
    heads = local_kv * group
    chunk = min(128, rows)
    slots = 2 * heads * (rows // chunk)
    vmem = pl.BlockSpec(memory_space=pltpu.VMEM)
    smem = pl.BlockSpec(memory_space=pltpu.SMEM)
    scores = heads * 2 * rows * keys.shape[0]
    return pl.pallas_call(
        functools.partial(attention_kernel, (rows, chunk, local_kv, group, value_dim)),
        out_shape=jax.ShapeDtypeStruct((rows, heads * value_dim), jnp.bfloat16),
        in_specs=[smem, smem, vmem, vmem, vmem],
        out_specs=vmem,
        scratch_shapes=[
            pltpu.VMEM((slots, chunk, 128), jnp.float32),
            pltpu.VMEM((slots, chunk, 128), jnp.float32),
            pltpu.VMEM((slots, chunk, value_dim), jnp.float32),
        ],
        compiler_params=pltpu.CompilerParams(vmem_limit_bytes=48 * 1024 * 1024),
        cost_estimate=pl.CostEstimate(
            flops=8 * scores * HEAD, bytes_accessed=keys.size * 2, transcendentals=scores
        ),
        name="attention",
    )(rank.reshape(1), lambdas, queries, keys, head_gain.reshape(1, value_dim))


def swap(rows, axis, size, distance):
    return lax.ppermute(rows, axis, [(i, i ^ distance) for i in range(size)])


def gather_near(block, axis, size):
    places = {0: block}
    distance = size // 2
    while distance:
        held = sorted(places)
        moved = swap(jnp.stack([places[p] for p in held]), axis, size, distance)
        places.update({p ^ distance: moved[i] for i, p in enumerate(held)})
        distance //= 2
    return jnp.stack([places[p] for p in range(size)])


def scatter_near(partials, axis, size):
    sums = {p: partials[p] for p in range(size)}
    distance = 1
    while distance < size:
        kept = [p for p in sorted(sums) if not p & distance]
        sent = jnp.stack([sums[p ^ distance].astype(jnp.bfloat16) for p in kept])
        moved = swap(sent, axis, size, distance).astype(jnp.float32)
        sums = {p: sums[p].astype(jnp.float32) + moved[i] for i, p in enumerate(kept)}
        distance *= 2
    return sums[0]


def exchange(blocks, axis, size):
    return [blocks[d] if d == 0 else swap(blocks[d], axis, size, d) for d in range(size)]


def body(
    mixer_input,
    mixer_gain,
    query_one,
    query_two,
    key_one,
    key_two,
    value_weight,
    lambdas,
    head_gain,
    output_weight,
    expert_input,
    expert_gain,
    routes,
    route_weight,
    expert_gate,
    expert_up,
    expert_down,
    shared_gate,
    shared_up,
    shared_down,
):
    ep_size = lax.axis_size("ep")
    tp_size = lax.axis_size("tp")
    ep_rank = lax.axis_index("ep")
    mixer_rows = mixer_input.shape[0]
    model_width = mixer_input.shape[1]
    query_cols = query_one.shape[1]
    key_cols = key_one.shape[1]
    value_dim = head_gain.shape[0]
    local_kv = key_cols // HEAD
    local_heads = query_cols // HEAD
    group_size = local_heads // local_kv
    normed = normalize(mixer_input, mixer_gain)
    joined_weight = jnp.concatenate([query_one, query_two, key_one, key_two, value_weight], axis=1)
    projected = jnp.dot(normed, joined_weight, preferred_element_type=jnp.float32).astype(
        jnp.bfloat16
    )
    query_part = projected[:, : 2 * query_cols]
    key_values = projected[:, 2 * query_cols :]
    arrived = lax.all_gather(key_values, "ep", axis=0, tiled=True)
    head_rows = attention(
        query_part, arrived, ep_rank, lambdas, head_gain, local_kv, group_size
    )
    mixer_partial = jnp.dot(head_rows, output_weight, preferred_element_type=jnp.float32).astype(
        jnp.bfloat16
    )
    tp_rank = lax.axis_index("tp")
    own_rows = mixer_rows // tp_size
    mixer_blocks = mixer_partial.reshape(tp_size, own_rows, model_width)
    mixer_sum = scatter_near(
        [
            lax.dynamic_index_in_dim(mixer_blocks, tp_rank ^ place, 0, keepdims=False)
            for place in range(tp_size)
        ],
        "tp",
        tp_size,
    ).astype(jnp.bfloat16)

    token_rows = expert_input.shape[0]
    normed_experts = normalize(expert_input, expert_gain)
    experts_local = expert_gate.shape[0]
    expert_count = experts_local * ep_size
    top_count = routes.shape[1]
    capacity = max(2, 5 * token_rows * top_count // (4 * expert_count))
    slot_count = expert_count * capacity
    direct = ep_size <= 16
    flat_routes = routes.reshape(-1)
    if direct:
        flat_routes = ((flat_routes // experts_local) ^ ep_rank) * experts_local + (
            flat_routes % experts_local
        )
    onehot = (flat_routes[:, None] == jnp.arange(expert_count, dtype=jnp.int32)[None, :]).astype(
        jnp.int32
    )
    slot_place = jnp.sum((jnp.cumsum(onehot, axis=0) - onehot) * onehot, axis=1)
    slot_ids = (flat_routes * capacity + slot_place).reshape(token_rows, top_count)
    slot_match = jnp.arange(slot_count, dtype=jnp.int32)[:, None, None] == slot_ids[None, :, :]
    select = jnp.any(slot_match, axis=2).astype(jnp.bfloat16)
    outgoing = jnp.dot(select, normed_experts, preferred_element_type=jnp.float32).astype(
        jnp.bfloat16
    )
    pair_rows = experts_local * capacity
    outgoing = outgoing.reshape(ep_size, pair_rows, model_width)
    if direct:
        received = exchange(outgoing, "ep", ep_size)
    else:
        received = list(lax.all_to_all(outgoing, "ep", split_axis=0, concat_axis=0, tiled=True))
    bundle = max(1, ep_size // GROUPS)
    expert_rows = gather_near(normed_experts, "tp", tp_size).reshape(-1, model_width)
    shared_gated = jnp.dot(expert_rows, shared_gate, preferred_element_type=jnp.float32)
    shared_lifted = jnp.dot(expert_rows, shared_up, preferred_element_type=jnp.float32)
    shared_hidden = (jax.nn.silu(shared_gated) * shared_lifted).astype(jnp.bfloat16)
    shared_part = (
        jnp.dot(shared_hidden, shared_down, preferred_element_type=jnp.float32)
        .astype(jnp.bfloat16)
        .reshape(tp_size, token_rows, model_width)
    )
    shared_result = scatter_near(shared_part, "tp", tp_size)
    results = []
    for begin in range(0, ep_size, bundle):
        held = jnp.stack(received[begin : begin + bundle])
        slot_rows = gather_near(held, "tp", tp_size).reshape(
            tp_size * bundle, experts_local, capacity, model_width
        )
        gated = jnp.einsum("secd,edf->secf", slot_rows, expert_gate, preferred_element_type=jnp.float32)
        lifted = jnp.einsum("secd,edf->secf", slot_rows, expert_up, preferred_element_type=jnp.float32)
        routed_hidden = (jax.nn.silu(gated) * lifted).astype(jnp.bfloat16)
        routed_part = (
            jnp.einsum(
                "secf,efd->secd", routed_hidden, expert_down, preferred_element_type=jnp.float32
            )
            .astype(jnp.bfloat16)
            .reshape(tp_size, bundle, pair_rows, model_width)
        )
        total = scatter_near(routed_part, "tp", tp_size).astype(jnp.bfloat16)
        results.extend(total[i] for i in range(bundle))
    if direct:
        returned = jnp.stack(exchange(results, "ep", ep_size))
    else:
        returned = lax.all_to_all(
            jnp.stack(results), "ep", split_axis=0, concat_axis=0, tiled=True
        )
    returned = returned.reshape(slot_count, model_width)
    spread = jnp.sum(
        jnp.where(
            jnp.arange(slot_count, dtype=jnp.int32)[None, None, :] == slot_ids[:, :, None],
            route_weight[:, :, None],
            0.0,
        ),
        axis=1,
    )
    upper = lax.reduce_precision(spread, 8, 7)
    lower = lax.reduce_precision(spread - upper, 8, 7)
    routed_total = jnp.dot(
        upper.astype(jnp.bfloat16), returned, preferred_element_type=jnp.float32
    ) + jnp.dot(lower.astype(jnp.bfloat16), returned, preferred_element_type=jnp.float32)
    expert_output = (routed_total + shared_result).astype(jnp.bfloat16)
    return (mixer_sum, expert_output)


def solution(mesh):
    in_specs = (
        P("ep", None),
        P(),
        P(None, "tp"),
        P(None, "tp"),
        P(None, "tp"),
        P(None, "tp"),
        P(None, "tp"),
        P("tp"),
        P(),
        P("tp", None),
        P(("ep", "tp"), None),
        P(),
        P(("ep", "tp"), None),
        P(("ep", "tp"), None),
        P("ep", None, "tp"),
        P("ep", None, "tp"),
        P("ep", "tp", None),
        P(None, "tp"),
        P(None, "tp"),
        P("tp", None),
    )
    out_specs = (P(("ep", "tp"), None), P(("ep", "tp"), None))
    return jax.shard_map(body, mesh=mesh, in_specs=in_specs, out_specs=out_specs, check_vma=False)
```

```python
import functools
import math

import jax
import jax.numpy as jnp
from jax import lax
from jax.experimental import pallas as pl
from jax.experimental.pallas import tpu as pltpu
from jax.sharding import PartitionSpec as P

HEAD = 64


EPS = 1e-06
NEG = -1e30


def normalize(activations, scaling):
    values = activations.astype(jnp.float32)
    factor = lax.rsqrt(jnp.mean(values * values, axis=-1, keepdims=True) + EPS)
    return (values * factor * scaling).astype(jnp.bfloat16)


def attention_kernel(
    shape, rank_ref, lambdas_ref, queries_ref, keys_ref, gain_ref, out_ref, maxima, totals, weighted
):
    rows, chunk, local_kv, group, value_dim = shape
    rank = rank_ref[0]
    maxima[...] = jnp.full(maxima.shape, NEG, jnp.float32)
    totals[...] = jnp.zeros(totals.shape, jnp.float32)
    weighted[...] = jnp.zeros(weighted.shape, jnp.float32)
    heads = local_kv * group
    key_cols = local_kv * HEAD
    chunks = rows // chunk
    scale = HEAD**-0.5 * math.log2(math.e)

    def block(index, masked):
        start = pl.multiple_of(index * rows, rows)
        for kv in range(local_kv):
            value_start = 2 * key_cols + kv * value_dim
            for part in range(chunks):
                span = (part + 1) * chunk if masked else rows
                values = keys_ref[pl.ds(start, span), value_start : value_start + value_dim]
                for which in range(2):
                    first = which * key_cols + kv * HEAD
                    keys = keys_ref[pl.ds(start, span), first : first + HEAD]
                    for g in range(group):
                        head = kv * group + g
                        col = (which * heads + head) * HEAD
                        queries = queries_ref[part * chunk : (part + 1) * chunk, col : col + HEAD]
                        scores = lax.dot_general(
                            queries,
                            keys,
                            (((1,), (1,)), ((), ())),
                            preferred_element_type=jnp.float32,
                        )
                        if masked:
                            row = part * chunk + lax.broadcasted_iota(jnp.int32, scores.shape, 0)
                            col_pos = lax.broadcasted_iota(jnp.int32, scores.shape, 1)
                            scores = jnp.where(col_pos <= row, scores, NEG)
                        slot = (which * heads + head) * chunks + part
                        earlier = maxima[slot]
                        latest = jnp.maximum(earlier, jnp.max(scores, axis=1, keepdims=True))
                        shrink = jnp.exp2((earlier - latest) * scale)
                        weights = jnp.exp2((scores - latest[:, :1]) * scale)
                        totals[slot] = totals[slot] * shrink + jnp.sum(
                            weights, axis=1, keepdims=True
                        )
                        weighted[slot] = weighted[slot] * shrink[:, :1] + jnp.dot(
                            weights.astype(jnp.bfloat16),
                            values,
                            preferred_element_type=jnp.float32,
                        )
                        maxima[slot] = latest

    def earlier_block(index, carry):
        block(index, False)
        return carry

    lax.fori_loop(0, rank, earlier_block, 0)
    block(rank, True)
    for head in range(heads):
        for part in range(chunks):
            one = head * chunks + part
            two = (heads + head) * chunks + part
            combined = (
                weighted[one] / totals[one][:, :1]
                - lambdas_ref[head] * (weighted[two] / totals[two][:, :1])
            )
            factor = lax.rsqrt(jnp.mean(combined * combined, axis=1, keepdims=True) + EPS)
            out_ref[
                part * chunk : (part + 1) * chunk, head * value_dim : (head + 1) * value_dim
            ] = (combined * factor * gain_ref[...]).astype(jnp.bfloat16)


def attention(queries, keys, rank, lambdas, head_gain, local_kv, group):
    rows = queries.shape[0]
    value_dim = head_gain.shape[0]
    heads = local_kv * group
    chunk = min(128, rows)
    slots = 2 * heads * (rows // chunk)
    vmem = pl.BlockSpec(memory_space=pltpu.VMEM)
    smem = pl.BlockSpec(memory_space=pltpu.SMEM)
    scores = heads * 2 * rows * keys.shape[0]
    return pl.pallas_call(
        functools.partial(attention_kernel, (rows, chunk, local_kv, group, value_dim)),
        out_shape=jax.ShapeDtypeStruct((rows, heads * value_dim), jnp.bfloat16),
        in_specs=[smem, smem, vmem, vmem, vmem],
        out_specs=vmem,
        scratch_shapes=[
            pltpu.VMEM((slots, chunk, 128), jnp.float32),
            pltpu.VMEM((slots, chunk, 128), jnp.float32),
            pltpu.VMEM((slots, chunk, value_dim), jnp.float32),
        ],
        compiler_params=pltpu.CompilerParams(vmem_limit_bytes=48 * 1024 * 1024),
        cost_estimate=pl.CostEstimate(
            flops=8 * scores * HEAD, bytes_accessed=keys.size * 2, transcendentals=scores
        ),
        name="attention",
    )(rank.reshape(1), lambdas, queries, keys, head_gain.reshape(1, value_dim))


def swap(rows, axis, size, distance):
    return lax.ppermute(rows, axis, [(i, i ^ distance) for i in range(size)])


def gather_near(block, axis, size):
    places = {0: block}
    distance = size // 2
    while distance:
        for place in sorted(places):
            places[place ^ distance] = swap(places[place], axis, size, distance)
        distance //= 2
    return [places[place] for place in range(size)]


def scatter_near(partials, axis, size):
    sums = dict(enumerate(partials))
    distance = 1
    while distance < size:
        kept = [place for place in sorted(sums) if not place & distance]
        moved = {
            place: swap(sums[place ^ distance].astype(jnp.bfloat16), axis, size, distance)
            for place in kept
        }
        sums = {
            place: sums[place].astype(jnp.float32) + moved[place].astype(jnp.float32)
            for place in kept
        }
        distance *= 2
    return sums[0]


def body(
    mixer_input,
    mixer_gain,
    query_one,
    query_two,
    key_one,
    key_two,
    value_weight,
    lambdas,
    head_gain,
    output_weight,
    expert_input,
    expert_gain,
    routes,
    route_weight,
    expert_gate,
    expert_up,
    expert_down,
    shared_gate,
    shared_up,
    shared_down,
):
    ep_size = lax.axis_size("ep")
    tp_size = lax.axis_size("tp")
    ep_rank = lax.axis_index("ep")
    mixer_rows = mixer_input.shape[0]
    model_width = mixer_input.shape[1]
    query_cols = query_one.shape[1]
    key_cols = key_one.shape[1]
    value_dim = head_gain.shape[0]
    local_kv = key_cols // HEAD
    local_heads = query_cols // HEAD
    group_size = local_heads // local_kv
    normed = normalize(mixer_input, mixer_gain)

    def project(weights):
        return jnp.concatenate(
            [
                jnp.dot(normed, weight, preferred_element_type=jnp.float32).astype(jnp.bfloat16)
                for weight in weights
            ],
            axis=1,
        )

    key_values = project([key_one, key_two, value_weight])
    query_part = project([query_one, query_two])
    arrived = lax.all_gather(key_values, "ep", axis=0, tiled=True)
    head_rows = attention(
        query_part, arrived, ep_rank, lambdas, head_gain, local_kv, group_size
    )
    tp_rank = lax.axis_index("tp")
    own_rows = mixer_rows // tp_size

    def mixer_place(place):
        rows = lax.dynamic_slice_in_dim(head_rows, (tp_rank ^ place) * own_rows, own_rows, 0)
        return jnp.dot(rows, output_weight, preferred_element_type=jnp.float32).astype(
            jnp.bfloat16
        )

    mixer_sum = scatter_near(
        [mixer_place(place) for place in range(tp_size)], "tp", tp_size
    ).astype(jnp.bfloat16)

    token_rows = expert_input.shape[0]
    normed_experts = normalize(expert_input, expert_gain)
    experts_local = expert_gate.shape[0]
    expert_count = experts_local * ep_size
    top_count = routes.shape[1]
    capacity = max(2, 5 * token_rows * top_count // (4 * expert_count))
    slot_count = expert_count * capacity
    flat_routes = routes.reshape(-1)
    onehot = (flat_routes[:, None] == jnp.arange(expert_count, dtype=jnp.int32)[None, :]).astype(
        jnp.int32
    )
    slot_place = jnp.sum((jnp.cumsum(onehot, axis=0) - onehot) * onehot, axis=1)
    slot_ids = (flat_routes * capacity + slot_place).reshape(token_rows, top_count)
    slot_match = jnp.arange(slot_count, dtype=jnp.int32)[:, None, None] == slot_ids[None, :, :]
    select = jnp.any(slot_match, axis=2).astype(jnp.bfloat16)
    outgoing = jnp.dot(select, normed_experts, preferred_element_type=jnp.float32).astype(
        jnp.bfloat16
    )
    pair_rows = experts_local * capacity
    outgoing = outgoing.reshape(ep_size, pair_rows, model_width)
    received = lax.all_to_all(outgoing, "ep", split_axis=0, concat_axis=0, tiled=True)
    received = received.reshape(ep_size, experts_local, capacity, model_width)
    if experts_local == 1:
        received = received.reshape(ep_size * capacity, model_width)

    def shared_expert(rows):
        gated = jnp.dot(rows, shared_gate, preferred_element_type=jnp.float32)
        lifted = jnp.dot(rows, shared_up, preferred_element_type=jnp.float32)
        hidden = (jax.nn.silu(gated) * lifted).astype(jnp.bfloat16)
        return jnp.dot(hidden, shared_down, preferred_element_type=jnp.float32).astype(
            jnp.bfloat16
        )

    def routed_expert(rows):
        if experts_local == 1:
            gated = jnp.dot(rows, expert_gate[0], preferred_element_type=jnp.float32)
            lifted = jnp.dot(rows, expert_up[0], preferred_element_type=jnp.float32)
            hidden = (jax.nn.silu(gated) * lifted).astype(jnp.bfloat16)
            return jnp.dot(hidden, expert_down[0], preferred_element_type=jnp.float32).astype(
                jnp.bfloat16
            )
        gated = jnp.einsum("secd,edf->secf", rows, expert_gate, preferred_element_type=jnp.float32)
        lifted = jnp.einsum("secd,edf->secf", rows, expert_up, preferred_element_type=jnp.float32)
        hidden = (jax.nn.silu(gated) * lifted).astype(jnp.bfloat16)
        return jnp.einsum(
            "secf,efd->secd", hidden, expert_down, preferred_element_type=jnp.float32
        ).astype(jnp.bfloat16)

    shared_places = gather_near(normed_experts, "tp", tp_size)
    routed_places = gather_near(received, "tp", tp_size)
    shared_result = scatter_near([shared_expert(rows) for rows in shared_places], "tp", tp_size)
    routed_result = scatter_near(
        [routed_expert(rows) for rows in routed_places], "tp", tp_size
    ).astype(jnp.bfloat16)
    returned = lax.all_to_all(
        routed_result.reshape(ep_size, pair_rows, model_width),
        "ep",
        split_axis=0,
        concat_axis=0,
        tiled=True,
    )
    returned = returned.reshape(slot_count, model_width)
    spread = jnp.sum(
        jnp.where(
            jnp.arange(slot_count, dtype=jnp.int32)[None, None, :] == slot_ids[:, :, None],
            route_weight[:, :, None],
            0.0,
        ),
        axis=1,
    )
    upper = lax.reduce_precision(spread, 8, 7)
    lower = lax.reduce_precision(spread - upper, 8, 7)
    routed_total = jnp.dot(
        upper.astype(jnp.bfloat16), returned, preferred_element_type=jnp.float32
    ) + jnp.dot(lower.astype(jnp.bfloat16), returned, preferred_element_type=jnp.float32)
    expert_output = (routed_total + shared_result).astype(jnp.bfloat16)
    return (mixer_sum, expert_output)


def solution(mesh):
    in_specs = (
        P("ep", None),
        P(),
        P(None, "tp"),
        P(None, "tp"),
        P(None, "tp"),
        P(None, "tp"),
        P(None, "tp"),
        P("tp"),
        P(),
        P("tp", None),
        P(("ep", "tp"), None),
        P(),
        P(("ep", "tp"), None),
        P(("ep", "tp"), None),
        P("ep", None, "tp"),
        P("ep", None, "tp"),
        P("ep", "tp", None),
        P(None, "tp"),
        P(None, "tp"),
        P("tp", None),
    )
    out_specs = (P(("ep", "tp"), None), P(("ep", "tp"), None))
    return jax.shard_map(body, mesh=mesh, in_specs=in_specs, out_specs=out_specs, check_vma=False)
```

```python
import functools
import math

import jax
import jax.numpy as jnp
from jax import lax
from jax.experimental import pallas as pl
from jax.experimental.pallas import tpu as pltpu
from jax.sharding import PartitionSpec as P

HEAD = 64


EPS = 1e-06
NEG = -1e30


def normalize(activations, scaling):
    values = activations.astype(jnp.float32)
    factor = lax.rsqrt(jnp.mean(values * values, axis=-1, keepdims=True) + EPS)
    return (values * factor * scaling).astype(jnp.bfloat16)


def attention_kernel(
    shape, rank_ref, lambdas_ref, queries_ref, keys_ref, gain_ref, out_ref, maxima, totals, weighted
):
    rows, chunk, local_kv, group, value_dim = shape
    rank = rank_ref[0]
    maxima[...] = jnp.full(maxima.shape, NEG, jnp.float32)
    totals[...] = jnp.zeros(totals.shape, jnp.float32)
    weighted[...] = jnp.zeros(weighted.shape, jnp.float32)
    heads = local_kv * group
    key_cols = local_kv * HEAD
    chunks = rows // chunk
    scale = HEAD**-0.5 * math.log2(math.e)

    def block(index, masked):
        start = pl.multiple_of(index * rows, rows)
        for kv in range(local_kv):
            value_start = 2 * key_cols + kv * value_dim
            for part in range(chunks):
                span = (part + 1) * chunk if masked else rows
                values = keys_ref[pl.ds(start, span), value_start : value_start + value_dim]
                for which in range(2):
                    first = which * key_cols + kv * HEAD
                    keys = keys_ref[pl.ds(start, span), first : first + HEAD]
                    for g in range(group):
                        head = kv * group + g
                        col = (which * heads + head) * HEAD
                        queries = queries_ref[part * chunk : (part + 1) * chunk, col : col + HEAD]
                        scores = lax.dot_general(
                            queries,
                            keys,
                            (((1,), (1,)), ((), ())),
                            preferred_element_type=jnp.float32,
                        )
                        if masked:
                            row = part * chunk + lax.broadcasted_iota(jnp.int32, scores.shape, 0)
                            col_pos = lax.broadcasted_iota(jnp.int32, scores.shape, 1)
                            scores = jnp.where(col_pos <= row, scores, NEG)
                        slot = (which * heads + head) * chunks + part
                        earlier = maxima[slot]
                        latest = jnp.maximum(earlier, jnp.max(scores, axis=1, keepdims=True))
                        shrink = jnp.exp2((earlier - latest) * scale)
                        weights = jnp.exp2((scores - latest[:, :1]) * scale)
                        totals[slot] = totals[slot] * shrink + jnp.sum(
                            weights, axis=1, keepdims=True
                        )
                        weighted[slot] = weighted[slot] * shrink[:, :1] + jnp.dot(
                            weights.astype(jnp.bfloat16),
                            values,
                            preferred_element_type=jnp.float32,
                        )
                        maxima[slot] = latest

    def earlier_block(index, carry):
        block(index, False)
        return carry

    lax.fori_loop(0, rank, earlier_block, 0)
    block(rank, True)
    for head in range(heads):
        for part in range(chunks):
            one = head * chunks + part
            two = (heads + head) * chunks + part
            combined = (
                weighted[one] / totals[one][:, :1]
                - lambdas_ref[head] * (weighted[two] / totals[two][:, :1])
            )
            factor = lax.rsqrt(jnp.mean(combined * combined, axis=1, keepdims=True) + EPS)
            out_ref[
                part * chunk : (part + 1) * chunk, head * value_dim : (head + 1) * value_dim
            ] = (combined * factor * gain_ref[...]).astype(jnp.bfloat16)


def attention(queries, keys, rank, lambdas, head_gain, local_kv, group):
    rows = queries.shape[0]
    value_dim = head_gain.shape[0]
    heads = local_kv * group
    chunk = min(128, rows)
    slots = 2 * heads * (rows // chunk)
    vmem = pl.BlockSpec(memory_space=pltpu.VMEM)
    smem = pl.BlockSpec(memory_space=pltpu.SMEM)
    scores = heads * 2 * rows * keys.shape[0]
    return pl.pallas_call(
        functools.partial(attention_kernel, (rows, chunk, local_kv, group, value_dim)),
        out_shape=jax.ShapeDtypeStruct((rows, heads * value_dim), jnp.bfloat16),
        in_specs=[smem, smem, vmem, vmem, vmem],
        out_specs=vmem,
        scratch_shapes=[
            pltpu.VMEM((slots, chunk, 128), jnp.float32),
            pltpu.VMEM((slots, chunk, 128), jnp.float32),
            pltpu.VMEM((slots, chunk, value_dim), jnp.float32),
        ],
        compiler_params=pltpu.CompilerParams(vmem_limit_bytes=48 * 1024 * 1024),
        cost_estimate=pl.CostEstimate(
            flops=8 * scores * HEAD, bytes_accessed=keys.size * 2, transcendentals=scores
        ),
        name="attention",
    )(rank.reshape(1), lambdas, queries, keys, head_gain.reshape(1, value_dim))


def swap(rows, axis, size, distance):
    return lax.ppermute(rows, axis, [(i, i ^ distance) for i in range(size)])


def gather_near(block, axis, size, ahead=None):
    places = {0: block}
    distance = size // 2
    while distance:
        for place in sorted(places):
            moved = swap(places[place], axis, size, distance)
            if ahead is not None:
                moved, ahead = lax.optimization_barrier((moved, ahead))
            places[place ^ distance] = moved
        ahead = None
        distance //= 2
    return [places[place] for place in range(size)]


def scatter_near(partials, axis, size):
    sums = dict(enumerate(partials))
    distance = 1
    while distance < size:
        kept = [place for place in sorted(sums) if not place & distance]
        moved = {
            place: swap(sums[place ^ distance].astype(jnp.bfloat16), axis, size, distance)
            for place in kept
        }
        sums = {
            place: sums[place].astype(jnp.float32) + moved[place].astype(jnp.float32)
            for place in kept
        }
        distance *= 2
    return sums[0]


def body(
    mixer_input,
    mixer_gain,
    query_one,
    query_two,
    key_one,
    key_two,
    value_weight,
    lambdas,
    head_gain,
    output_weight,
    expert_input,
    expert_gain,
    routes,
    route_weight,
    expert_gate,
    expert_up,
    expert_down,
    shared_gate,
    shared_up,
    shared_down,
):
    ep_size = lax.axis_size("ep")
    tp_size = lax.axis_size("tp")
    ep_rank = lax.axis_index("ep")
    mixer_rows = mixer_input.shape[0]
    model_width = mixer_input.shape[1]
    query_cols = query_one.shape[1]
    key_cols = key_one.shape[1]
    value_dim = head_gain.shape[0]
    local_kv = key_cols // HEAD
    local_heads = query_cols // HEAD
    group_size = local_heads // local_kv
    normed = normalize(mixer_input, mixer_gain)

    def project(weights):
        return jnp.concatenate(
            [
                jnp.dot(normed, weight, preferred_element_type=jnp.float32).astype(jnp.bfloat16)
                for weight in weights
            ],
            axis=1,
        )

    key_values = project([key_one, key_two, value_weight])
    query_part = project([query_one, query_two])
    arrived = lax.all_gather(key_values, "ep", axis=0, tiled=True)
    head_rows = attention(
        query_part, arrived, ep_rank, lambdas, head_gain, local_kv, group_size
    )
    tp_rank = lax.axis_index("tp")
    own_rows = mixer_rows // tp_size

    def mixer_place(place):
        rows = lax.dynamic_slice_in_dim(head_rows, (tp_rank ^ place) * own_rows, own_rows, 0)
        return jnp.dot(rows, output_weight, preferred_element_type=jnp.float32).astype(
            jnp.bfloat16
        )

    mixer_sum = scatter_near(
        [mixer_place(place) for place in range(tp_size)], "tp", tp_size
    ).astype(jnp.bfloat16)

    token_rows = expert_input.shape[0]
    normed_experts = normalize(expert_input, expert_gain)
    experts_local = expert_gate.shape[0]
    expert_count = experts_local * ep_size
    top_count = routes.shape[1]
    capacity = max(2, 5 * token_rows * top_count // (4 * expert_count))
    slot_count = expert_count * capacity
    flat_routes = routes.reshape(-1)
    onehot = (flat_routes[:, None] == jnp.arange(expert_count, dtype=jnp.int32)[None, :]).astype(
        jnp.int32
    )
    slot_place = jnp.sum((jnp.cumsum(onehot, axis=0) - onehot) * onehot, axis=1)
    slot_ids = (flat_routes * capacity + slot_place).reshape(token_rows, top_count)
    slot_match = jnp.arange(slot_count, dtype=jnp.int32)[:, None, None] == slot_ids[None, :, :]
    select = jnp.any(slot_match, axis=2).astype(jnp.bfloat16)
    outgoing = jnp.dot(select, normed_experts, preferred_element_type=jnp.float32).astype(
        jnp.bfloat16
    )
    pair_rows = experts_local * capacity
    outgoing = outgoing.reshape(ep_size, pair_rows, model_width)
    outgoing, key_values = lax.optimization_barrier((outgoing, key_values))
    received = lax.all_to_all(outgoing, "ep", split_axis=0, concat_axis=0, tiled=True)
    received = received.reshape(ep_size, experts_local, capacity, model_width)
    if experts_local == 1:
        received = received.reshape(ep_size * capacity, model_width)

    def shared_expert(rows):
        gated = jnp.dot(rows, shared_gate, preferred_element_type=jnp.float32)
        lifted = jnp.dot(rows, shared_up, preferred_element_type=jnp.float32)
        hidden = (jax.nn.silu(gated) * lifted).astype(jnp.bfloat16)
        return jnp.dot(hidden, shared_down, preferred_element_type=jnp.float32).astype(
            jnp.bfloat16
        )

    def routed_expert(rows):
        if experts_local == 1:
            gated = jnp.dot(rows, expert_gate[0], preferred_element_type=jnp.float32)
            lifted = jnp.dot(rows, expert_up[0], preferred_element_type=jnp.float32)
            hidden = (jax.nn.silu(gated) * lifted).astype(jnp.bfloat16)
            return jnp.dot(hidden, expert_down[0], preferred_element_type=jnp.float32).astype(
                jnp.bfloat16
            )
        gated = jnp.einsum("secd,edf->secf", rows, expert_gate, preferred_element_type=jnp.float32)
        lifted = jnp.einsum("secd,edf->secf", rows, expert_up, preferred_element_type=jnp.float32)
        hidden = (jax.nn.silu(gated) * lifted).astype(jnp.bfloat16)
        return jnp.einsum(
            "secf,efd->secd", hidden, expert_down, preferred_element_type=jnp.float32
        ).astype(jnp.bfloat16)

    shared_places = gather_near(normed_experts, "tp", tp_size)
    routed_places = gather_near(received, "tp", tp_size, head_rows)
    shared_result = scatter_near([shared_expert(rows) for rows in shared_places], "tp", tp_size)
    routed_result = scatter_near(
        [routed_expert(rows) for rows in routed_places], "tp", tp_size
    ).astype(jnp.bfloat16)
    returned = lax.all_to_all(
        routed_result.reshape(ep_size, pair_rows, model_width),
        "ep",
        split_axis=0,
        concat_axis=0,
        tiled=True,
    )
    returned = returned.reshape(slot_count, model_width)
    spread = jnp.sum(
        jnp.where(
            jnp.arange(slot_count, dtype=jnp.int32)[None, None, :] == slot_ids[:, :, None],
            route_weight[:, :, None],
            0.0,
        ),
        axis=1,
    )
    upper = lax.reduce_precision(spread, 8, 7)
    lower = lax.reduce_precision(spread - upper, 8, 7)
    routed_total = jnp.dot(
        upper.astype(jnp.bfloat16), returned, preferred_element_type=jnp.float32
    ) + jnp.dot(lower.astype(jnp.bfloat16), returned, preferred_element_type=jnp.float32)
    expert_output = (routed_total + shared_result).astype(jnp.bfloat16)
    return (mixer_sum, expert_output)


def solution(mesh):
    in_specs = (
        P("ep", None),
        P(),
        P(None, "tp"),
        P(None, "tp"),
        P(None, "tp"),
        P(None, "tp"),
        P(None, "tp"),
        P("tp"),
        P(),
        P("tp", None),
        P(("ep", "tp"), None),
        P(),
        P(("ep", "tp"), None),
        P(("ep", "tp"), None),
        P("ep", None, "tp"),
        P("ep", None, "tp"),
        P("ep", "tp", None),
        P(None, "tp"),
        P(None, "tp"),
        P("tp", None),
    )
    out_specs = (P(("ep", "tp"), None), P(("ep", "tp"), None))
    return jax.shard_map(body, mesh=mesh, in_specs=in_specs, out_specs=out_specs, check_vma=False)
```
